32 devices in a mesh: grp: 2 (over y), dp: 2 (over x), kv: 4 (over z), tp: 2 (over core).
Axes of the slice: x: 2, y: 2, z: 4, core: 2. Of those that a mesh axis runs over, the one named last changes fastest.
Arguments:
- tokens: bfloat16 [128, 2048], P(('grp', 'dp'), ('kv', 'tp')), parts along dimension 0, may hold values from -6 to 6
- norm_gain: float32 [2048], P('kv'), may hold values from 0.1 to 1.9
- w_query: bfloat16 [2048, 512], P('kv', 'tp'), may hold values from -0.125 to 0.125
- w_key: bfloat16 [2048, 512], P('kv', 'tp'), may hold values from -0.125 to 0.125
- w_value: bfloat16 [2048, 1024], P('kv', 'tp'), may hold values from -0.125 to 0.125
- w_outgate: bfloat16 [2048, 1024], P('kv', 'tp'), may hold values from -0.125 to 0.125
- w_ingate: bfloat16 [2048, 8], P('kv'), may hold values from -0.125 to 0.125
- w_forget: bfloat16 [2048, 8], P('kv'), may hold values from -0.125 to 0.125
- in_bias: float32 [8], replicated, may hold values from -1.5 to 0.5
- forget_bias: float32 [8], replicated, may hold values from -1 to 4
- memory: float32 [128, 8, 64, 128], P(('grp', 'dp', 'kv'), 'tp'), parts along dimension 0, may hold values from -4 to 4
- normalizer: float32 [128, 512], P(('grp', 'dp', 'kv'), 'tp'), parts along dimension 0, may hold values from -4 to 4
- stabilizer: float32 [128, 8], P(('grp', 'dp', 'kv'), 'tp'), parts along dimension 0, may hold values from -1 to 1
- w_out: bfloat16 [1024, 2048], P('tp', 'kv'), may hold values from -0.1875 to 0.1875
- mlp_gain: float32 [2048], replicated, may hold values from 0.1 to 1.9
- w_up: bfloat16 [2048, 8192], P(None, ('kv', 'tp')), may hold values from -0.125 to 0.125
- w_down: bfloat16 [8192, 2048], P(('kv', 'tp')), may hold values from -0.09375 to 0.09375
Outputs:
- mixed_out: bfloat16 [128, 2048], P(('grp', 'dp'), ('kv', 'tp')), parts along dimension 0
- memory_new: float32 [128, 8, 64, 128], P(('grp', 'dp', 'kv'), 'tp'), parts along dimension 0
- normalizer_new: float32 [128, 512], P(('grp', 'dp', 'kv'), 'tp'), parts along dimension 0
- stabilizer_new: float32 [128, 8], P(('grp', 'dp', 'kv'), 'tp'), parts along dimension 0
The draws below stay inside these ranges and needn't reach their ends.
There are 2 independent parts, one for each index of `grp`. The reference program is written for one: setup_inputs(seed, part) draws one part's arguments, and reference() takes and returns one part's arrays. A program takes and returns all parts, laid end to end along the dimension named above; an argument that names none is the same for every part. Nothing has to cross between parts.
All inputs are finite; a program needn't handle non-finite values.
Results may differ from the reference program's by a relative error of at most 0.03.
Values may be sent and summed in bfloat16 or wider, within the bound.
A program may use at most 64 MiB of HBM per device.

```python
import jax
import jax.numpy as jnp
from jax import lax

D = 2048
HEADS = 8
QK_DIM = 64
VD_DIM = 128
FF = 8192
BATCH = 64
N_KV = 4
N_TP = 2


def with_spikes(drawn, stream_key, source, target, blocks, factor):
    owner, partner = [(jnp.arange(drawn.shape[dim]) // (drawn.shape[dim] // blocks)).reshape([-1 if axis == dim else 1 for axis in range(drawn.ndim)]) for dim in (source, target)]
    chosen = jax.random.permutation(stream_key, blocks)[partner]
    strong = (owner == chosen) | (owner == (partner + blocks // 2) % blocks)
    return jnp.where(strong, factor * drawn, drawn)


def block_levels(key, dims, cuts, smallest, largest):
    def one(dim, shards_of):
        heights = jax.random.uniform(jax.random.fold_in(jax.random.fold_in(key, 6), dim), (shards_of,), jnp.float32, smallest / len(cuts), largest / len(cuts))
        return jnp.repeat(jnp.exp(heights), dims[dim] // shards_of).reshape((-1,) + (1,) * (len(dims) - dim - 1))

    loudness = one(*cuts[0])
    for cut in cuts[1:]:
        loudness = loudness * one(*cut)
    return loudness


def bell_draw(own_key, shape, scale, most, split=(), held_as=jnp.bfloat16):
    gain = block_levels(own_key, shape, split, -0.22, 0.18) if split else 1.0
    result = jax.random.normal(own_key, shape, jnp.float32) * scale * gain
    return jnp.minimum(jnp.maximum(result, -most), most).astype(held_as)


def noise_with(key, dims, scale, most, cuts, heavy, dtype=jnp.bfloat16):
    values = scale * jax.random.normal(key, dims, jnp.float32)
    if cuts:
        values = values * block_levels(key, dims, cuts, -0.22, 0.18)
    return jnp.clip(with_spikes(values, jax.random.fold_in(key, 3), *heavy), -most, most).astype(dtype)


def setup_inputs(seed: int = 0, part: int = 0) -> dict:
    key_of = jax.random.split(jax.random.key(seed), 18)
    part_splits = jax.random.split(jax.random.fold_in(key_of[17], part), 18)
    tokens = noise_with(part_splits[0], (BATCH, D), 1.0, 6.0, ((0, 2), (1, 8)), (1, 0, 8, 2.0))
    norm_gain = jnp.clip(1.0 + 0.18 * jax.random.normal(key_of[1], (D,), jnp.float32), 0.1, 1.9)
    w_query = bell_draw(key_of[2], (D, HEADS * QK_DIM), D ** -0.5, 0.125, ((0, 4), (1, 2)))
    w_key = bell_draw(key_of[3], (D, HEADS * QK_DIM), D ** -0.5, 0.125, ((0, 4), (1, 2)))
    w_value = bell_draw(key_of[4], (D, HEADS * VD_DIM), D ** -0.5, 0.125, ((0, 4), (1, 2)))
    w_outgate = bell_draw(key_of[5], (D, HEADS * VD_DIM), D ** -0.5, 0.125, ((0, 4), (1, 2)))
    w_ingate = bell_draw(key_of[6], (D, HEADS), D ** -0.5, 0.125, ((0, 4),))
    w_forget = bell_draw(key_of[7], (D, HEADS), D ** -0.5, 0.125, ((0, 4),))
    in_bias = jnp.clip(jax.random.uniform(key_of[8], (HEADS,), jnp.float32, -1.5, 0.5), -1.5, 0.5)
    forget_bias = jnp.clip(jax.random.uniform(key_of[9], (HEADS,), jnp.float32, -1.0, 4.0), -1.0, 4.0)
    memory = bell_draw(part_splits[10], (BATCH, HEADS, QK_DIM, VD_DIM), 0.5, 4.0, ((0, 8), (1, 2)), jnp.float32)
    normalizer = bell_draw(part_splits[11], (BATCH, HEADS * QK_DIM), 0.5, 4.0, ((0, 8), (1, 2)), jnp.float32)
    stabilizer = jnp.clip(jax.random.uniform(part_splits[12], (BATCH, HEADS), jnp.float32, -1.0, 1.0) * block_levels(part_splits[12], (BATCH, HEADS), ((0, 8), (1, 2)), -0.4, 0.0), -1.0, 1.0)
    w_out = bell_draw(key_of[13], (HEADS * VD_DIM, D), (HEADS * VD_DIM) ** -0.5, 0.1875, ((0, 2), (1, 4)))
    mlp_gain = jnp.clip(1.0 + 0.18 * jax.random.normal(key_of[14], (D,), jnp.float32), 0.1, 1.9)
    w_up = bell_draw(key_of[15], (D, FF), D ** -0.5, 0.125, ((1, 8),))
    w_down = noise_with(key_of[16], (FF, D), FF ** -0.5, 0.09375, ((0, 8),), (0, 1, 8, 2.0))
    return dict(tokens=tokens, norm_gain=norm_gain, w_query=w_query, w_key=w_key, w_value=w_value, w_outgate=w_outgate, w_ingate=w_ingate, w_forget=w_forget, in_bias=in_bias, forget_bias=forget_bias, memory=memory, normalizer=normalizer, stabilizer=stabilizer, w_out=w_out, mlp_gain=mlp_gain, w_up=w_up, w_down=w_down)


EPSILON = 1e-06

def block_sum(left, weight, parts):
    rows = left.shape[0]
    width = weight.shape[0] // parts
    left_blocks = jnp.transpose(left.reshape(rows, parts, width), (1, 0, 2))
    weight_blocks = weight.reshape(parts, width, weight.shape[1])

    def step(total, pair):
        term = jnp.dot(pair[0], pair[1], preferred_element_type=jnp.float32).astype(jnp.bfloat16)
        term = lax.optimization_barrier(term)
        return (total + term.astype(jnp.float32), None)
    start = jnp.zeros((rows, weight.shape[1]), jnp.float32)
    total, unused = lax.scan(step, start, (left_blocks, weight_blocks))
    return total

def reference(tokens, norm_gain, w_query, w_key, w_value, w_outgate, w_ingate, w_forget, in_bias, forget_bias, memory, normalizer, stabilizer, w_out, mlp_gain, w_up, w_down):
    batch_rows = tokens.shape[0]
    tokens_f = tokens.astype(jnp.float32)
    rscale = lax.rsqrt(lax.optimization_barrier(jnp.mean(tokens_f * tokens_f, axis=1, keepdims=True)) + EPSILON)
    scaled = (tokens_f * norm_gain).astype(jnp.bfloat16)

    def product(weight):
        return block_sum(scaled, weight, N_KV) * rscale
    queries = product(w_query).reshape(batch_rows, HEADS, QK_DIM)
    keys_in = (product(w_key) * QK_DIM ** (-0.5)).reshape(batch_rows, HEADS, QK_DIM)
    values_in = product(w_value).reshape(batch_rows, HEADS, VD_DIM)
    out_pre = product(w_outgate).reshape(batch_rows, HEADS, VD_DIM)
    log_in = product(w_ingate) + in_bias
    log_forget = jax.nn.log_sigmoid(product(w_forget) + forget_bias)
    carried = log_forget + stabilizer
    stab_new = jnp.maximum(carried, log_in)
    take_new = jnp.exp(log_in - stab_new)
    keep_old = jnp.exp(carried - stab_new)
    norm_old = normalizer.reshape(batch_rows, HEADS, QK_DIM)
    score = lax.optimization_barrier(jnp.sum(queries * keys_in, axis=2))
    readout = jnp.einsum('shkv,shk->shv', memory, queries, precision=lax.Precision.HIGHEST)
    numer = (take_new * score)[..., None] * values_in + keep_old[..., None] * readout
    denom = take_new * score + keep_old * lax.optimization_barrier(jnp.sum(norm_old * queries, axis=2))
    cell = numer / jnp.maximum(jnp.abs(denom), 1.0)[..., None]
    hidden = (jax.nn.sigmoid(out_pre) * cell).reshape(batch_rows, HEADS * VD_DIM).astype(jnp.bfloat16)
    middle = (tokens_f + jnp.dot(hidden, w_out, preferred_element_type=jnp.float32)).astype(jnp.bfloat16)
    middle_f = middle.astype(jnp.float32)
    rscale_mid = lax.rsqrt(lax.optimization_barrier(jnp.mean(middle_f * middle_f, axis=1, keepdims=True)) + EPSILON)
    normed = (middle_f * rscale_mid * mlp_gain).astype(jnp.bfloat16)
    upward = jnp.dot(normed, w_up, preferred_element_type=jnp.float32)
    squared = jnp.square(jax.nn.relu(upward)).astype(jnp.bfloat16)
    mixed_out = (middle_f + block_sum(squared, w_down, N_KV * N_TP)).astype(jnp.bfloat16)
    memory_new = keep_old[..., None, None] * memory + take_new[..., None, None] * keys_in[..., :, None] * values_in[..., None, :]
    normalizer_new = (keep_old[..., None] * norm_old + take_new[..., None] * keys_in).reshape(batch_rows, HEADS * QK_DIM)
    return (mixed_out, memory_new, normalizer_new, stab_new)
```

```python
import functools

import jax
import jax.numpy as jnp
from jax import lax
from jax.experimental import pallas as pl
from jax.experimental.pallas import tpu as pltpu
from jax.sharding import PartitionSpec as P

EPSILON = 1e-06
F32 = jnp.float32
BF16 = jnp.bfloat16
MESH = pl.DeviceIdType.MESH
LANES = 128


def far_first(count):
    return sorted(range(1, count), key=lambda d: (-min(d, count - d), d))


def step_kernel(
    n_kv,
    n_tp,
    tokens,
    norm_gain,
    w_query,
    w_key,
    w_value,
    w_outgate,
    w_ingate,
    w_forget,
    in_bias,
    forget_bias,
    memory,
    normalizer,
    stabilizer,
    w_out,
    mlp_gain,
    w_up,
    w_down,
    mixed_out,
    memory_new,
    normalizer_new,
    stabilizer_new,
    tok,
    ngain,
    wq,
    wk,
    wv,
    wg,
    wi,
    wf,
    bias_i,
    bias_f,
    mem,
    nrm,
    stab,
    wo,
    mgain,
    wu,
    wd,
    part_out,
    part_in,
    gate_out,
    gate_in,
    readout,
    hid,
    mid,
    wide,
    down_out,
    down_in,
    mem_out,
    nrm_out,
    stab_out,
    mix_out,
    load_sem,
    store_sem,
    tok_send,
    tok_recv,
    wo_send,
    wo_recv,
    part_send,
    part_recv,
    gate_send,
    gate_recv,
    hid_send,
    hid_recv,
    mid_send,
    mid_recv,
    down_send,
    down_recv,
):
    kv = lax.axis_index("kv")
    tp = lax.axis_index("tp")
    me = kv * n_tp + tp
    rows, width = tokens.shape
    seqs, heads, qk, vd = memory.shape
    model_width = mlp_gain.shape[1]
    aligned = width % LANES == 0
    n_all = n_kv * n_tp

    def load(index, src, dst):
        copy = pltpu.make_async_copy(src, dst, load_sem.at[index])
        copy.start()
        return copy

    if aligned:
        own_cols = pl.ds(pl.multiple_of(tp * width, LANES), width)
        wo_local = w_out.at[:, own_cols]
    else:
        wo_local = w_out
    get_tok = load(0, tokens, tok.at[tp])
    get_ngain = load(1, norm_gain, ngain)
    get_proj = [
        load(2 + i, src, dst)
        for i, (src, dst) in enumerate(
            [
                (w_query, wq),
                (w_key, wk),
                (w_value, wv),
                (w_outgate, wg),
                (w_ingate, wi),
                (w_forget, wf),
            ]
        )
    ]
    get_cell = [
        load(8 + i, src, dst)
        for i, (src, dst) in enumerate(
            [
                (in_bias, bias_i),
                (forget_bias, bias_f),
                (stabilizer, stab),
                (normalizer, nrm),
                (memory, mem),
            ]
        )
    ]
    get_wo = load(13, wo_local, wo.at[tp])
    get_mgain = load(14, mlp_gain, mgain)
    get_up = load(15, w_up, wu)
    get_down = load(16, w_down, wd)

    offsets = [(dk, dt) for dk in far_first(n_kv) for dt in range(n_tp)]
    offsets += [(0, dt) for dt in range(1, n_tp)]

    def peer(dk, dt):
        return lax.rem(kv + dk, n_kv), lax.rem(tp + dt, n_tp)

    barrier = pltpu.get_barrier_semaphore()
    for dk, dt in offsets:
        pk, pt = peer(dk, dt)
        pl.semaphore_signal(barrier, inc=1, device_id={"kv": pk, "tp": pt}, device_id_type=MESH)
    get_tok.wait()
    pl.semaphore_wait(barrier, len(offsets))

    def remote(src, dst, send, recv, pk, pt):
        return pltpu.make_async_remote_copy(
            src_ref=src,
            dst_ref=dst,
            send_sem=send,
            recv_sem=recv,
            device_id={"kv": pk, "tp": pt},
            device_id_type=MESH,
        )

    sends = []
    for dt in range(1, n_tp):
        pt = lax.rem(tp + dt, n_tp)
        copy = remote(tok.at[tp], tok.at[tp], tok_send.at[dt], tok_recv.at[tp], kv, pt)
        copy.start()
        sends.append(copy)
    for dt in range(1, n_tp):
        pt = lax.rem(tp + dt, n_tp)
        if aligned:
            src = w_out.at[:, pl.ds(pl.multiple_of(pt * width, LANES), width)]
        else:
            src = w_out
        copy = remote(src, wo.at[tp], wo_send.at[dt], wo_recv.at[tp], kv, pt)
        copy.start()
        sends.append(copy)
    get_ngain.wait()
    for copy in get_proj:
        copy.wait()
    for dt in range(1, n_tp):
        pt = lax.rem(tp + dt, n_tp)
        remote(tok.at[pt], tok.at[pt], tok_send.at[dt], tok_recv.at[pt], kv, pt).wait_recv()

    scaled = []
    squares = jnp.zeros((rows, 1), F32)
    for t in range(n_tp):
        block = tok[t].astype(F32)
        squares = squares + jnp.sum(block * block, axis=1, keepdims=True)
        scaled.append((block * ngain[:, t * width : (t + 1) * width]).astype(BF16))

    def product(weight):
        total = None
        for t in range(n_tp):
            term = jnp.dot(
                scaled[t],
                weight[t * width : (t + 1) * width, :],
                preferred_element_type=F32,
            )
            total = term if total is None else total + term
        return total

    q_wide, v_wide = wq.shape[1], wv.shape[1]
    col = 0
    spans = []
    for weight in (wq, wk, wv, wg):
        acc = product(weight)
        span = (col, col + weight.shape[1])
        spans.append(span)
        for j in range(n_kv):
            part_out[j, :, span[0] : span[1]] = acc[j * seqs : (j + 1) * seqs].astype(BF16)
        col = span[1]
    all_heads = wi.shape[1]
    acc_i = product(wi)
    acc_f = product(wf)
    for j in range(n_kv):
        cut = slice(j * seqs, (j + 1) * seqs)
        gate_out[j] = jnp.zeros((seqs, gate_out.shape[2]), F32)
        gate_out[j, :, 0:all_heads] = acc_i[cut]
        gate_out[j, :, all_heads : 2 * all_heads] = acc_f[cut]
        gate_out[j, :, 2 * all_heads : 2 * all_heads + 1] = squares[cut]
    for dk in far_first(n_kv):
        pk = lax.rem(kv + dk, n_kv)
        for out, into, s_sem, r_sem in (
            (gate_out, gate_in, gate_send, gate_recv),
            (part_out, part_in, part_send, part_recv),
        ):
            copy = remote(out.at[pk], into.at[kv], s_sem.at[dk], r_sem.at[kv], pk, tp)
            copy.start()
            sends.append(copy)
    total = part_out[kv].astype(F32)
    gates = gate_out[kv]
    for copy in get_cell:
        copy.wait()
    for dk in reversed(far_first(n_kv)):
        pk = lax.rem(kv + dk, n_kv)
        remote(gate_out.at[pk], gate_in.at[pk], gate_send.at[dk], gate_recv.at[pk], pk, tp).wait_recv()
        remote(part_out.at[pk], part_in.at[pk], part_send.at[dk], part_recv.at[pk], pk, tp).wait_recv()
        total = total + part_in[pk].astype(F32)
        gates = gates + gate_in[pk]

    row_scale = lax.rsqrt(gates[:, 2 * all_heads : 2 * all_heads + 1] / model_width + EPSILON)
    total = total * row_scale
    queries = total[:, spans[0][0] : spans[0][1]]
    keys_in = total[:, spans[1][0] : spans[1][1]] * (qk**-0.5)
    values_in = total[:, spans[2][0] : spans[2][1]]
    out_pre = total[:, spans[3][0] : spans[3][1]]
    gates = gates * row_scale
    pre_i = gates[:, 0:all_heads] + bias_i[...]
    pre_f = gates[:, all_heads : 2 * all_heads] + bias_f[...]
    log_in = pre_i[:, 0:heads]
    forget_arg = pre_f[:, 0:heads]
    for t in range(1, n_tp):
        log_in = jnp.where(tp == t, pre_i[:, t * heads : (t + 1) * heads], log_in)
        forget_arg = jnp.where(tp == t, pre_f[:, t * heads : (t + 1) * heads], forget_arg)
    log_forget = jnp.minimum(forget_arg, 0.0) - jnp.log1p(jnp.exp(-jnp.abs(forget_arg)))
    carried = log_forget + stab[...]
    stab_now = jnp.maximum(carried, log_in)
    take_new = jnp.exp(log_in - stab_now)
    keep_old = jnp.exp(carried - stab_now)
    stab_out[...] = stab_now
    norm_old = nrm[...]

    q_cols = jnp.transpose(queries)
    for h in range(heads):
        for s in range(seqs):
            column = q_cols[h * qk : (h + 1) * qk, s : s + 1]
            readout[s : s + 1, h * vd : (h + 1) * vd] = jnp.sum(mem[s, h] * column, axis=0, keepdims=True)
    keep_rows, take_rows = [], []
    for h in range(heads):
        k_cut = slice(h * qk, (h + 1) * qk)
        v_cut = slice(h * vd, (h + 1) * vd)
        take = take_new[:, h : h + 1]
        keep = keep_old[:, h : h + 1]
        score = jnp.sum(queries[:, k_cut] * keys_in[:, k_cut], axis=1, keepdims=True)
        past = jnp.sum(norm_old[:, k_cut] * queries[:, k_cut], axis=1, keepdims=True)
        numer = (take * score) * values_in[:, v_cut] + keep * readout[:, v_cut]
        denom = take * score + keep * past
        cell = numer / jnp.maximum(jnp.abs(denom), 1.0)
        hid[me, :, v_cut] = (jax.nn.sigmoid(out_pre[:, v_cut]) * cell).astype(BF16)
        keep_rows.append(jnp.broadcast_to(keep, (seqs, vd)))
        take_rows.append(take * values_in[:, v_cut])
    for i, (dk, dt) in enumerate(offsets):
        pk, pt = peer(dk, dt)
        copy = remote(hid.at[me], hid.at[me], hid_send.at[i], hid_recv.at[me], pk, pt)
        copy.start()
        sends.append(copy)

    k_cols = jnp.transpose(keys_in)
    stores = []
    for s in range(seqs):
        for h in range(heads):
            column = k_cols[h * qk : (h + 1) * qk, s : s + 1]
            mem_out[s, h] = keep_rows[h][s : s + 1] * mem[s, h] + column * take_rows[h][s : s + 1]
    for h in range(heads):
        k_cut = slice(h * qk, (h + 1) * qk)
        nrm_out[:, k_cut] = (
            keep_old[:, h : h + 1] * norm_old[:, k_cut] + take_new[:, h : h + 1] * keys_in[:, k_cut]
        )
    for i, (src, dst) in enumerate(
        [(mem_out, memory_new), (nrm_out, normalizer_new), (stab_out, stabilizer_new)]
    ):
        copy = pltpu.make_async_copy(src, dst, store_sem.at[i])
        copy.start()
        stores.append(copy)

    get_wo.wait()
    for dt in range(1, n_tp):
        pt = lax.rem(tp + dt, n_tp)
        remote(wo.at[pt], wo.at[pt], wo_send.at[dt], wo_recv.at[pt], kv, pt).wait_recv()
    for i, (dk, dt) in reversed(list(enumerate(offsets))):
        pk, pt = peer(dk, dt)
        src = pk * n_tp + pt
        remote(hid.at[src], hid.at[src], hid_send.at[i], hid_recv.at[src], pk, pt).wait_recv()
    projected = None
    for t in range(n_tp):
        lhs = jnp.concatenate([hid[k * n_tp + t].astype(F32) for k in range(n_kv)], axis=0)
        term = jnp.dot(lhs.astype(BF16), wo[t], preferred_element_type=F32)
        projected = term if projected is None else projected + term
    if not aligned:
        picked = projected[:, 0:width]
        for t in range(1, n_tp):
            picked = jnp.where(tp == t, projected[:, t * width : (t + 1) * width], picked)
        projected = picked
    middle = (tok[tp].astype(F32) + projected).astype(BF16)
    mid[me] = middle
    for i, (dk, dt) in enumerate(offsets):
        pk, pt = peer(dk, dt)
        copy = remote(mid.at[me], mid.at[me], mid_send.at[i], mid_recv.at[me], pk, pt)
        copy.start()
        sends.append(copy)

    get_mgain.wait()
    get_up.wait()
    arrivals = [(None, (0, 0))] + list(reversed(list(enumerate(offsets))))
    upward = None
    energy = None
    for i, (dk, dt) in arrivals:
        pk, pt = peer(dk, dt)
        src = pk * n_tp + pt
        if i is not None:
            remote(mid.at[src], mid.at[src], mid_send.at[i], mid_recv.at[src], pk, pt).wait_recv()
        if aligned:
            block = middle.astype(F32) if i is None else mid[src].astype(F32)
            gain = mgain[:, pl.ds(pl.multiple_of(src * width, LANES), width)]
            lhs = (block * gain).astype(BF16)
            weight = wu[pl.ds(pl.multiple_of(src * width, LANES), width), :]
            term = jnp.dot(lhs, weight, preferred_element_type=F32)
            upward = term if upward is None else upward + term
            energy = block * block if energy is None else energy + block * block
    if aligned:
        energy = jnp.sum(energy, axis=1, keepdims=True)
    else:
        for j in range(n_all):
            wide[:, j * width : (j + 1) * width] = mid[j].astype(F32)
        block = wide[...]
        energy = jnp.sum(block * block, axis=1, keepdims=True)
        upward = jnp.dot((block * mgain[...]).astype(BF16), wu[...], preferred_element_type=F32)
    mid_scale = lax.rsqrt(energy / model_width + EPSILON)
    squared = jnp.square(jnp.maximum(upward * mid_scale, 0.0)).astype(BF16)

    get_down.wait()
    if not aligned:
        partial = jnp.dot(squared, wd[...], preferred_element_type=F32)
        for j in range(n_all):
            down_out[j] = partial[:, j * width : (j + 1) * width].astype(BF16)
    for i, (dk, dt) in enumerate(offsets):
        pk, pt = peer(dk, dt)
        dst = pk * n_tp + pt
        if aligned:
            weight = wd[:, pl.ds(pl.multiple_of(dst * width, LANES), width)]
            down_out[dst] = jnp.dot(squared, weight, preferred_element_type=F32).astype(BF16)
        copy = remote(down_out.at[dst], down_in.at[me], down_send.at[i], down_recv.at[me], pk, pt)
        copy.start()
        sends.append(copy)
    if aligned:
        weight = wd[:, pl.ds(pl.multiple_of(me * width, LANES), width)]
        branch = jnp.dot(squared, weight, preferred_element_type=F32)
    else:
        branch = down_out[me].astype(F32)
    branch = branch + middle.astype(F32)
    for i, (dk, dt) in reversed(list(enumerate(offsets))):
        pk, pt = peer(dk, dt)
        src = pk * n_tp + pt
        remote(down_out.at[src], down_in.at[src], down_send.at[i], down_recv.at[src], pk, pt).wait_recv()
        branch = branch + down_in[src].astype(F32)
    mix_out[...] = branch.astype(BF16)
    last = pltpu.make_async_copy(mix_out, mixed_out, store_sem.at[3])
    last.start()
    stores.append(last)
    for copy in sends:
        copy.wait_send()
    for copy in stores:
        copy.wait()


def shards(
    n_kv,
    n_tp,
    tokens,
    norm_gain,
    w_query,
    w_key,
    w_value,
    w_outgate,
    w_ingate,
    w_forget,
    in_bias,
    forget_bias,
    memory,
    normalizer,
    stabilizer,
    w_out,
    mlp_gain,
    w_up,
    w_down,
):
    rows, width = tokens.shape
    seqs, heads, qk, vd = memory.shape
    n_all = n_kv * n_tp
    aligned = width % LANES == 0
    proj = w_query.shape[1] + w_key.shape[1] + w_value.shape[1] + w_outgate.shape[1]
    hidden = heads * vd
    out_cols = width if aligned else w_out.shape[1]
    model_width = mlp_gain.shape[0]
    gate_lanes = -(-(2 * w_ingate.shape[1] + 1) // LANES) * LANES
    operands = (
        tokens,
        norm_gain.reshape(1, -1),
        w_query,
        w_key,
        w_value,
        w_outgate,
        w_ingate,
        w_forget,
        in_bias.reshape(1, -1),
        forget_bias.reshape(1, -1),
        memory,
        normalizer,
        stabilizer,
        w_out,
        mlp_gain.reshape(1, -1),
        w_up,
        w_down,
    )
    anywhere = pl.BlockSpec(memory_space=pl.ANY)

    def like(ref):
        return pltpu.VMEM(ref.shape, ref.dtype)

    dma = pltpu.SemaphoreType.DMA
    scratch = [
        pltpu.VMEM((n_tp, rows, width), BF16),
        like(operands[1]),
        like(w_query),
        like(w_key),
        like(w_value),
        like(w_outgate),
        like(w_ingate),
        like(w_forget),
        like(operands[8]),
        like(operands[9]),
        like(memory),
        like(normalizer),
        like(stabilizer),
        pltpu.VMEM((n_tp, w_out.shape[0], out_cols), BF16),
        like(operands[14]),
        like(w_up),
        like(w_down),
        pltpu.VMEM((n_kv, seqs, proj), BF16),
        pltpu.VMEM((n_kv, seqs, proj), BF16),
        pltpu.VMEM((n_kv, seqs, gate_lanes), F32),
        pltpu.VMEM((n_kv, seqs, gate_lanes), F32),
        pltpu.VMEM((seqs, hidden), F32),
        pltpu.VMEM((n_all, seqs, hidden), BF16),
        pltpu.VMEM((n_all, rows, width), BF16),
        pltpu.VMEM((8, LANES) if aligned else (rows, model_width), F32),
        pltpu.VMEM((n_all, rows, width), BF16),
        pltpu.VMEM((n_all, rows, width), BF16),
        like(memory),
        like(normalizer),
        like(stabilizer),
        like(tokens),
        dma((17,)),
        dma((4,)),
        dma((n_tp,)),
        dma((n_tp,)),
        dma((n_tp,)),
        dma((n_tp,)),
        dma((n_kv,)),
        dma((n_kv,)),
        dma((n_kv,)),
        dma((n_kv,)),
        dma((n_all,)),
        dma((n_all,)),
        dma((n_all,)),
        dma((n_all,)),
        dma((n_all,)),
        dma((n_all,)),
    ]
    return pl.pallas_call(
        functools.partial(step_kernel, n_kv, n_tp),
        out_shape=(
            jax.ShapeDtypeStruct(tokens.shape, tokens.dtype),
            jax.ShapeDtypeStruct(memory.shape, memory.dtype),
            jax.ShapeDtypeStruct(normalizer.shape, normalizer.dtype),
            jax.ShapeDtypeStruct(stabilizer.shape, stabilizer.dtype),
        ),
        in_specs=[anywhere] * len(operands),
        out_specs=(anywhere,) * 4,
        scratch_shapes=scratch,
        compiler_params=pltpu.CompilerParams(
            collective_id=0, has_side_effects=True, vmem_limit_bytes=56 * 1024 * 1024
        ),
    )(*operands)


def solution(mesh):
    placed = (
        P(("grp", "dp"), ("kv", "tp")),
        P("kv"),
        P("kv", "tp"),
        P("kv", "tp"),
        P("kv", "tp"),
        P("kv", "tp"),
        P("kv", None),
        P("kv", None),
        P(),
        P(),
        P(("grp", "dp", "kv"), "tp", None, None),
        P(("grp", "dp", "kv"), "tp"),
        P(("grp", "dp", "kv"), "tp"),
        P("tp", "kv"),
        P(),
        P(None, ("kv", "tp")),
        P(("kv", "tp"), None),
    )
    return jax.shard_map(
        functools.partial(shards, mesh.shape["kv"], mesh.shape["tp"]),
        mesh=mesh,
        in_specs=placed,
        out_specs=(
            P(("grp", "dp"), ("kv", "tp")),
            P(("grp", "dp", "kv"), "tp", None, None),
            P(("grp", "dp", "kv"), "tp"),
            P(("grp", "dp", "kv"), "tp"),
        ),
        check_vma=False,
    )
```

```python
import functools

import jax
import jax.numpy as jnp
from jax import lax
from jax.experimental import pallas as pl
from jax.experimental.pallas import tpu as pltpu
from jax.sharding import PartitionSpec as P

EPSILON = 1e-06
F32 = jnp.float32
BF16 = jnp.bfloat16
MESH = pl.DeviceIdType.MESH
LANES = 128


def far_first(count):
    return sorted(range(1, count), key=lambda d: (-min(d, count - d), d))


def step_kernel(
    n_kv,
    n_tp,
    tokens,
    norm_gain,
    w_query,
    w_key,
    w_value,
    w_outgate,
    w_ingate,
    w_forget,
    in_bias,
    forget_bias,
    memory,
    normalizer,
    stabilizer,
    w_out,
    mlp_gain,
    w_up,
    w_down,
    mixed_out,
    memory_new,
    normalizer_new,
    stabilizer_new,
    tok,
    ngain,
    wq,
    wk,
    wv,
    wg,
    wi,
    wf,
    bias_i,
    bias_f,
    mem,
    nrm,
    stab,
    wo,
    mgain,
    wu,
    wd,
    part_out,
    part_in,
    late_out,
    late_in,
    gate_out,
    gate_in,
    readout,
    hid,
    mid,
    wide,
    down_out,
    down_in,
    load_sem,
    tok_send,
    tok_recv,
    wo_send,
    wo_recv,
    part_send,
    part_recv,
    late_send,
    late_recv,
    gate_send,
    gate_recv,
    hid_send,
    hid_recv,
    mid_send,
    mid_recv,
    down_send,
    down_recv,
):
    kv = lax.axis_index("kv")
    tp = lax.axis_index("tp")
    me = kv * n_tp + tp
    rows, width = tokens.shape
    seqs, heads, qk, vd = memory.shape
    model_width = mlp_gain.shape[1]
    aligned = width % LANES == 0
    n_all = n_kv * n_tp

    def load(index, src, dst):
        copy = pltpu.make_async_copy(src, dst, load_sem.at[index])
        copy.start()
        return copy

    if aligned:
        own_cols = pl.ds(pl.multiple_of(tp * width, LANES), width)
        wo_local = w_out.at[:, own_cols]
    else:
        wo_local = w_out
    get_tok = load(0, tokens, tok.at[tp])
    get_ngain = load(1, norm_gain, ngain)
    get_proj = [
        load(2 + i, src, dst)
        for i, (src, dst) in enumerate(
            [
                (w_query, wq),
                (w_key, wk),
                (w_value, wv),
                (w_outgate, wg),
                (w_ingate, wi),
                (w_forget, wf),
            ]
        )
    ]
    get_cell = [
        load(8 + i, src, dst)
        for i, (src, dst) in enumerate(
            [
                (in_bias, bias_i),
                (forget_bias, bias_f),
                (stabilizer, stab),
                (normalizer, nrm),
                (memory, mem),
            ]
        )
    ]
    get_wo = load(13, wo_local, wo.at[tp])
    get_mgain = load(14, mlp_gain, mgain)
    get_up = load(15, w_up, wu)
    get_down = load(16, w_down, wd)

    offsets = [(dk, dt) for dk in far_first(n_kv) for dt in range(n_tp)]
    offsets += [(0, dt) for dt in range(1, n_tp)]

    def peer(dk, dt):
        return lax.rem(kv + dk, n_kv), lax.rem(tp + dt, n_tp)

    barrier = pltpu.get_barrier_semaphore()
    for dk, dt in offsets:
        pk, pt = peer(dk, dt)
        pl.semaphore_signal(barrier, inc=1, device_id={"kv": pk, "tp": pt}, device_id_type=MESH)
    get_tok.wait()
    pl.semaphore_wait(barrier, len(offsets))

    def remote(src, dst, send, recv, pk, pt):
        return pltpu.make_async_remote_copy(
            src_ref=src,
            dst_ref=dst,
            send_sem=send,
            recv_sem=recv,
            device_id={"kv": pk, "tp": pt},
            device_id_type=MESH,
        )

    sends = []
    for dt in range(1, n_tp):
        pt = lax.rem(tp + dt, n_tp)
        copy = remote(tok.at[tp], tok.at[tp], tok_send.at[dt], tok_recv.at[tp], kv, pt)
        copy.start()
        sends.append(copy)
    for dt in range(1, n_tp):
        pt = lax.rem(tp + dt, n_tp)
        if aligned:
            src = w_out.at[:, pl.ds(pl.multiple_of(pt * width, LANES), width)]
        else:
            src = w_out
        copy = remote(src, wo.at[tp], wo_send.at[dt], wo_recv.at[tp], kv, pt)
        copy.start()
        sends.append(copy)
    get_ngain.wait()
    for copy in get_proj:
        copy.wait()
    for dt in range(1, n_tp):
        pt = lax.rem(tp + dt, n_tp)
        remote(tok.at[pt], tok.at[pt], tok_send.at[dt], tok_recv.at[pt], kv, pt).wait_recv()

    scaled = []
    squares = jnp.zeros((rows, 1), F32)
    for t in range(n_tp):
        block = tok[t].astype(F32)
        squares = squares + jnp.sum(block * block, axis=1, keepdims=True)
        scaled.append((block * ngain[:, t * width : (t + 1) * width]).astype(BF16))

    def product(weight):
        total = None
        for t in range(n_tp):
            term = jnp.dot(
                scaled[t],
                weight[t * width : (t + 1) * width, :],
                preferred_element_type=F32,
            )
            total = term if total is None else total + term
        return total

    def turned(weight):
        total = None
        for t in range(n_tp):
            term = lax.dot_general(
                scaled[t],
                weight[:, t * width : (t + 1) * width],
                (((1,), (1,)), ((), ())),
                preferred_element_type=F32,
            )
            total = term if total is None else total + term
        return total

    def scatter(out, into, s_sem, r_sem):
        for dk in far_first(n_kv):
            pk = lax.rem(kv + dk, n_kv)
            copy = remote(out.at[pk], into.at[kv], s_sem.at[dk], r_sem.at[kv], pk, tp)
            copy.start()
            sends.append(copy)

    def collect(total, out, into, s_sem, r_sem):
        for dk in reversed(far_first(n_kv)):
            pk = lax.rem(kv + dk, n_kv)
            remote(out.at[pk], into.at[pk], s_sem.at[dk], r_sem.at[pk], pk, tp).wait_recv()
            total = total + into[pk].astype(F32)
        return total

    all_heads = wi.shape[0]
    acc_i = turned(wi)
    acc_f = turned(wf)
    for j in range(n_kv):
        cut = slice(j * seqs, (j + 1) * seqs)
        gate_out[j, :, 0:all_heads] = acc_i[cut]
        gate_out[j, :, all_heads : 2 * all_heads] = acc_f[cut]
        gate_out[j, :, 2 * all_heads : 2 * all_heads + 1] = squares[cut]
    scatter(gate_out, gate_in, gate_send, gate_recv)
    for weights, out in (((wq, wk), part_out), ((wv, wg), late_out)):
        col = 0
        for weight in weights:
            acc = product(weight)
            end = col + weight.shape[1]
            for j in range(n_kv):
                out[j, :, col:end] = acc[j * seqs : (j + 1) * seqs].astype(BF16)
            col = end
        if out is part_out:
            scatter(part_out, part_in, part_send, part_recv)
        else:
            scatter(late_out, late_in, late_send, late_recv)
    for copy in get_cell:
        copy.wait()
    gates = collect(gate_out[kv], gate_out, gate_in, gate_send, gate_recv)
    early = collect(part_out[kv].astype(F32), part_out, part_in, part_send, part_recv)

    row_scale = lax.rsqrt(gates[:, 2 * all_heads : 2 * all_heads + 1] / model_width + EPSILON)
    early = early * row_scale
    queries = early[:, 0 : heads * qk]
    keys_in = early[:, heads * qk :] * (qk**-0.5)
    gates = gates * row_scale
    pre_i = gates[:, 0:all_heads] + bias_i[...]
    pre_f = gates[:, all_heads : 2 * all_heads] + bias_f[...]
    log_in = pre_i[:, 0:heads]
    forget_arg = pre_f[:, 0:heads]
    for t in range(1, n_tp):
        log_in = jnp.where(tp == t, pre_i[:, t * heads : (t + 1) * heads], log_in)
        forget_arg = jnp.where(tp == t, pre_f[:, t * heads : (t + 1) * heads], forget_arg)
    log_forget = jnp.minimum(forget_arg, 0.0) - jnp.log1p(jnp.exp(-jnp.abs(forget_arg)))
    carried = log_forget + jnp.transpose(stab[...])
    stab_now = jnp.maximum(carried, log_in)
    take_new = jnp.exp(log_in - stab_now)
    keep_old = jnp.exp(carried - stab_now)
    stabilizer_new[...] = jnp.transpose(stab_now)
    norm_old = nrm[...]

    q_cols = jnp.transpose(queries)
    for h in range(heads):
        for s in range(seqs):
            column = q_cols[h * qk : (h + 1) * qk, s : s + 1]
            readout[s : s + 1, h * vd : (h + 1) * vd] = jnp.sum(mem[s, h] * column, axis=0, keepdims=True)
    late = collect(late_out[kv].astype(F32), late_out, late_in, late_send, late_recv)
    late = late * row_scale
    values_in = late[:, 0 : heads * vd]
    out_pre = late[:, heads * vd :]
    keep_rows, take_rows = [], []
    for h in range(heads):
        k_cut = slice(h * qk, (h + 1) * qk)
        v_cut = slice(h * vd, (h + 1) * vd)
        take = take_new[:, h : h + 1]
        keep = keep_old[:, h : h + 1]
        score = jnp.sum(queries[:, k_cut] * keys_in[:, k_cut], axis=1, keepdims=True)
        past = jnp.sum(norm_old[:, k_cut] * queries[:, k_cut], axis=1, keepdims=True)
        numer = (take * score) * values_in[:, v_cut] + keep * readout[:, v_cut]
        denom = take * score + keep * past
        cell = numer / jnp.maximum(jnp.abs(denom), 1.0)
        hid[me, :, v_cut] = (jax.nn.sigmoid(out_pre[:, v_cut]) * cell).astype(BF16)
        keep_rows.append(jnp.broadcast_to(keep, (seqs, vd)))
        take_rows.append(take * values_in[:, v_cut])
    for i, (dk, dt) in enumerate(offsets):
        pk, pt = peer(dk, dt)
        copy = remote(hid.at[me], hid.at[me], hid_send.at[i], hid_recv.at[me], pk, pt)
        copy.start()
        sends.append(copy)

    k_cols = jnp.transpose(keys_in)
    for s in range(seqs):
        for h in range(heads):
            column = k_cols[h * qk : (h + 1) * qk, s : s + 1]
            memory_new[s, h] = keep_rows[h][s : s + 1] * mem[s, h] + column * take_rows[h][s : s + 1]
    for h in range(heads):
        k_cut = slice(h * qk, (h + 1) * qk)
        normalizer_new[:, k_cut] = (
            keep_old[:, h : h + 1] * norm_old[:, k_cut] + take_new[:, h : h + 1] * keys_in[:, k_cut]
        )
    get_wo.wait()
    for dt in range(1, n_tp):
        pt = lax.rem(tp + dt, n_tp)
        remote(wo.at[pt], wo.at[pt], wo_send.at[dt], wo_recv.at[pt], kv, pt).wait_recv()
    for i, (dk, dt) in reversed(list(enumerate(offsets))):
        pk, pt = peer(dk, dt)
        src = pk * n_tp + pt
        remote(hid.at[src], hid.at[src], hid_send.at[i], hid_recv.at[src], pk, pt).wait_recv()
    projected = None
    for t in range(n_tp):
        lhs = jnp.concatenate([hid[k * n_tp + t].astype(F32) for k in range(n_kv)], axis=0)
        term = jnp.dot(lhs.astype(BF16), wo[t], preferred_element_type=F32)
        projected = term if projected is None else projected + term
    if not aligned:
        picked = projected[:, 0:width]
        for t in range(1, n_tp):
            picked = jnp.where(tp == t, projected[:, t * width : (t + 1) * width], picked)
        projected = picked
    middle = (tok[tp].astype(F32) + projected).astype(BF16)
    mid[me] = middle
    for i, (dk, dt) in enumerate(offsets):
        pk, pt = peer(dk, dt)
        copy = remote(mid.at[me], mid.at[me], mid_send.at[i], mid_recv.at[me], pk, pt)
        copy.start()
        sends.append(copy)

    get_mgain.wait()
    get_up.wait()
    arrivals = [(None, (0, 0))] + list(reversed(list(enumerate(offsets))))
    upward = None
    energy = None
    for i, (dk, dt) in arrivals:
        pk, pt = peer(dk, dt)
        src = pk * n_tp + pt
        if i is not None:
            remote(mid.at[src], mid.at[src], mid_send.at[i], mid_recv.at[src], pk, pt).wait_recv()
        if aligned:
            block = middle.astype(F32) if i is None else mid[src].astype(F32)
            gain = mgain[:, pl.ds(pl.multiple_of(src * width, LANES), width)]
            lhs = (block * gain).astype(BF16)
            weight = wu[pl.ds(pl.multiple_of(src * width, LANES), width), :]
            term = jnp.dot(lhs, weight, preferred_element_type=F32)
            upward = term if upward is None else upward + term
            energy = block * block if energy is None else energy + block * block
    if aligned:
        energy = jnp.sum(energy, axis=1, keepdims=True)
    else:
        for j in range(n_all):
            wide[:, j * width : (j + 1) * width] = mid[j].astype(F32)
        block = wide[...]
        energy = jnp.sum(block * block, axis=1, keepdims=True)
        upward = jnp.dot((block * mgain[...]).astype(BF16), wu[...], preferred_element_type=F32)
    mid_scale = lax.rsqrt(energy / model_width + EPSILON)
    squared = jnp.square(jnp.maximum(upward * mid_scale, 0.0)).astype(BF16)

    get_down.wait()
    if not aligned:
        partial = jnp.dot(squared, wd[...], preferred_element_type=F32)
        for j in range(n_all):
            down_out[j] = partial[:, j * width : (j + 1) * width].astype(BF16)
    for i, (dk, dt) in enumerate(offsets):
        pk, pt = peer(dk, dt)
        dst = pk * n_tp + pt
        if aligned:
            weight = wd[:, pl.ds(pl.multiple_of(dst * width, LANES), width)]
            down_out[dst] = jnp.dot(squared, weight, preferred_element_type=F32).astype(BF16)
        copy = remote(down_out.at[dst], down_in.at[me], down_send.at[i], down_recv.at[me], pk, pt)
        copy.start()
        sends.append(copy)
    if aligned:
        weight = wd[:, pl.ds(pl.multiple_of(me * width, LANES), width)]
        branch = jnp.dot(squared, weight, preferred_element_type=F32)
    else:
        branch = down_out[me].astype(F32)
    branch = branch + middle.astype(F32)
    for i, (dk, dt) in reversed(list(enumerate(offsets))):
        pk, pt = peer(dk, dt)
        src = pk * n_tp + pt
        remote(down_out.at[src], down_in.at[src], down_send.at[i], down_recv.at[src], pk, pt).wait_recv()
        branch = branch + down_in[src].astype(F32)
    mixed_out[...] = branch.astype(BF16)
    for copy in sends:
        copy.wait_send()


def store_kernel(*refs):
    count = (len(refs) - 1) // 2
    sem = refs[-1]
    copies = [
        pltpu.make_async_copy(refs[i], refs[count + i], sem.at[i]) for i in range(count)
    ]
    for copy in copies:
        copy.start()
    for copy in copies:
        copy.wait()


def shards(
    n_kv,
    n_tp,
    tokens,
    norm_gain,
    w_query,
    w_key,
    w_value,
    w_outgate,
    w_ingate,
    w_forget,
    in_bias,
    forget_bias,
    memory,
    normalizer,
    stabilizer,
    w_out,
    mlp_gain,
    w_up,
    w_down,
):
    rows, width = tokens.shape
    seqs, heads, qk, vd = memory.shape
    n_all = n_kv * n_tp
    aligned = width % LANES == 0
    early = w_query.shape[1] + w_key.shape[1]
    late = w_value.shape[1] + w_outgate.shape[1]
    hidden = heads * vd
    out_cols = width if aligned else w_out.shape[1]
    model_width = mlp_gain.shape[0]
    gate_lanes = -(-(2 * w_ingate.shape[1] + 1) // LANES) * LANES
    operands = (
        tokens,
        norm_gain.reshape(1, -1),
        w_query,
        w_key,
        w_value,
        w_outgate,
        w_ingate.T,
        w_forget.T,
        in_bias.reshape(1, -1),
        forget_bias.reshape(1, -1),
        memory,
        normalizer,
        stabilizer.T,
        w_out,
        mlp_gain.reshape(1, -1),
        w_up,
        w_down,
    )
    anywhere = pl.BlockSpec(memory_space=pl.ANY)

    def like(ref):
        return pltpu.VMEM(ref.shape, ref.dtype)

    dma = pltpu.SemaphoreType.DMA
    scratch = [
        pltpu.VMEM((n_tp, rows, width), BF16),
        like(operands[1]),
        like(w_query),
        like(w_key),
        like(w_value),
        like(w_outgate),
        like(operands[6]),
        like(operands[7]),
        like(operands[8]),
        like(operands[9]),
        like(memory),
        like(normalizer),
        like(operands[12]),
        pltpu.VMEM((n_tp, w_out.shape[0], out_cols), BF16),
        like(operands[14]),
        like(w_up),
        like(w_down),
        pltpu.VMEM((n_kv, seqs, early), BF16),
        pltpu.VMEM((n_kv, seqs, early), BF16),
        pltpu.VMEM((n_kv, seqs, late), BF16),
        pltpu.VMEM((n_kv, seqs, late), BF16),
        pltpu.VMEM((n_kv, seqs, gate_lanes), F32),
        pltpu.VMEM((n_kv, seqs, gate_lanes), F32),
        pltpu.VMEM((seqs, hidden), F32),
        pltpu.VMEM((n_all, seqs, hidden), BF16),
        pltpu.VMEM((n_all, rows, width), BF16),
        pltpu.VMEM((8, LANES) if aligned else (rows, model_width), F32),
        pltpu.VMEM((n_all, rows, width), BF16),
        pltpu.VMEM((n_all, rows, width), BF16),
        dma((17,)),
        dma((n_tp,)),
        dma((n_tp,)),
        dma((n_tp,)),
        dma((n_tp,)),
        dma((n_kv,)),
        dma((n_kv,)),
        dma((n_kv,)),
        dma((n_kv,)),
        dma((n_kv,)),
        dma((n_kv,)),
        dma((n_all,)),
        dma((n_all,)),
        dma((n_all,)),
        dma((n_all,)),
        dma((n_all,)),
        dma((n_all,)),
    ]
    shapes = tuple(
        jax.ShapeDtypeStruct(a.shape, a.dtype)
        for a in (tokens, memory, normalizer, operands[12])
    )
    in_vmem = (pl.BlockSpec(memory_space=pltpu.VMEM),) * len(shapes)
    held = pl.pallas_call(
        functools.partial(step_kernel, n_kv, n_tp),
        out_shape=tuple(pltpu.VMEM(a.shape, a.dtype) for a in shapes),
        in_specs=[anywhere] * len(operands),
        out_specs=in_vmem,
        scratch_shapes=scratch,
        compiler_params=pltpu.CompilerParams(
            collective_id=0, has_side_effects=True, vmem_limit_bytes=56 * 1024 * 1024
        ),
    )(*operands)
    mixed_out, memory_new, normalizer_new, stab_new = pl.pallas_call(
        store_kernel,
        out_shape=shapes,
        in_specs=in_vmem,
        out_specs=(anywhere,) * len(shapes),
        scratch_shapes=[dma((len(shapes),))],
    )(*[pltpu.with_memory_space_constraint(a, pltpu.VMEM) for a in held])
    return (mixed_out, memory_new, normalizer_new, stab_new.T)


def solution(mesh):
    placed = (
        P(("grp", "dp"), ("kv", "tp")),
        P("kv"),
        P("kv", "tp"),
        P("kv", "tp"),
        P("kv", "tp"),
        P("kv", "tp"),
        P("kv", None),
        P("kv", None),
        P(),
        P(),
        P(("grp", "dp", "kv"), "tp", None, None),
        P(("grp", "dp", "kv"), "tp"),
        P(("grp", "dp", "kv"), "tp"),
        P("tp", "kv"),
        P(),
        P(None, ("kv", "tp")),
        P(("kv", "tp"), None),
    )
    return jax.shard_map(
        functools.partial(shards, mesh.shape["kv"], mesh.shape["tp"]),
        mesh=mesh,
        in_specs=placed,
        out_specs=(
            P(("grp", "dp"), ("kv", "tp")),
            P(("grp", "dp", "kv"), "tp", None, None),
            P(("grp", "dp", "kv"), "tp"),
            P(("grp", "dp", "kv"), "tp"),
        ),
        check_vma=False,
    )
```
